32 devices in a mesh: rep: 2 (over x), fs: 8 (over z, y), tp: 2 (over core).
Axes of the slice: x: 2, y: 2, z: 4, core: 2. Of those that a mesh axis runs over, the one named last changes fastest.
Arguments:
- tokens: bfloat16 [256, 16, 2048], P('tp', ('rep', 'fs')), may hold values from -6 to 6
- mix_gain: float32 [2048], replicated, may hold values from 0.1 to 1.9
- value_weight: bfloat16 [2048, 1024], P('fs', 'tp'), may hold values from -0.125 to 0.125
- gate_weight: bfloat16 [2048, 1024], P('fs', 'tp'), may hold values from -0.125 to 0.125
- conv_taps: float32 [31, 1024], P(None, 'tp'), may hold values from -1 to 1
- head_gain: float32 [1024], P('tp'), may hold values from 0.1 to 1.9
- out_weight: bfloat16 [1024, 2048], P('tp', 'fs'), may hold values from -0.1875 to 0.1875
- ffn_gain: float32 [2048], replicated, may hold values from 0.1 to 1.9
- ffn_gate_weight: bfloat16 [2048, 3072], P('fs', 'tp'), may hold values from -0.125 to 0.125
- ffn_up_weight: bfloat16 [2048, 3072], P('fs', 'tp'), may hold values from -0.125 to 0.125
- down_weight: bfloat16 [3072, 2048], P('tp', 'fs'), may hold values from -0.109375 to 0.109375
Outputs:
- layer_out: bfloat16 [256, 16, 2048], P('tp', ('rep', 'fs'))
The draws below stay inside these ranges and needn't reach their ends.
All inputs are finite; a program needn't handle non-finite values.
Results may differ from the reference program's by a relative error of at most 0.012.
Values may be sent and summed in bfloat16 or wider, within the bound.
A program may use at most 128 MiB of HBM per device.

```python
import jax
import jax.numpy as jnp
from jax import lax

D = 2048
HEADS = 8
HEAD_DIM = 128
FF = 3072
KW = 31
LEN = 256
SEQ_DEV = 1
CH = 1024
BATCH = 16
N_TP = 2


def block_levels(stream_key, dims, pieces, low, high):
    loudness = 1.0
    for axis_at, parts in pieces:
        heights = jax.random.uniform(jax.random.fold_in(jax.random.fold_in(stream_key, 6), axis_at), (parts,), jnp.float32, low / len(pieces), high / len(pieces))
        loudness = loudness * jnp.repeat(jnp.exp(heights), dims[axis_at] // parts).reshape((-1,) + (1,) * (len(dims) - 1 - axis_at))
    return loudness


def centred(stream_key, extent, deviation, bound, shards=(), kind=jnp.bfloat16):
    gain = block_levels(stream_key, extent, shards, -0.22, 0.18) if shards else 1.0
    drawn = jax.random.normal(stream_key, extent, jnp.float32) * deviation * gain
    return jnp.minimum(jnp.maximum(drawn, -bound), bound).astype(kind)


def setup_inputs(seed: int = 0) -> dict:
    keys = jax.random.split(jax.random.key(seed), 12)
    return {
        "tokens": centred(keys[0], (LEN, BATCH, D), 1.0, 6.0, ((0, 2), (1, 16))),
        "mix_gain": jnp.clip(1.0 + 0.18 * jax.random.normal(keys[1], (D,), jnp.float32), 0.1, 1.9),
        "value_weight": centred(keys[2], (D, CH), D ** -0.5, 0.125, ((0, 8), (1, 2))),
        "gate_weight": centred(keys[3], (D, CH), D ** -0.5, 0.125, ((0, 8), (1, 2))),
        "conv_taps": centred(keys[4], (KW, CH), KW ** -0.5, 1.0, ((1, 2),), jnp.float32),
        "head_gain": jnp.clip(1.0 + 0.18 * jax.random.normal(keys[5], (CH,), jnp.float32), 0.1, 1.9),
        "out_weight": centred(keys[6], (CH, D), CH ** -0.5, 0.1875, ((0, 2), (1, 8))),
        "ffn_gain": jnp.clip(1.0 + 0.18 * jax.random.normal(keys[7], (D,), jnp.float32), 0.1, 1.9),
        "ffn_gate_weight": centred(keys[8], (D, FF), D ** -0.5, 0.125, ((0, 8), (1, 2))),
        "ffn_up_weight": centred(keys[9], (D, FF), D ** -0.5, 0.125, ((0, 8), (1, 2))),
        "down_weight": centred(keys[10], (FF, D), FF ** -0.5, 0.109375, ((0, 2), (1, 8))),
    }


norm_eps = 1e-06
group_eps = 1e-05

def rms_scale(matrix, scales):
    return matrix * lax.rsqrt(lax.optimization_barrier(jnp.mean(matrix * matrix, axis=-1, keepdims=True)) + norm_eps) * scales

def split_sum(activated, weights, block_width):
    summed = jnp.zeros((activated.shape[0], weights.shape[1]), jnp.float32)
    for block_idx in range(N_TP):
        lower = block_idx * block_width
        partial_value = jnp.dot(activated[:, lower:lower + block_width], weights[lower:lower + block_width], preferred_element_type=jnp.float32).astype(jnp.bfloat16)
        partial_value = lax.optimization_barrier(partial_value)
        summed = summed + partial_value.astype(jnp.float32)
    return summed

def reference(tokens, mix_gain, value_weight, gate_weight, conv_taps, head_gain, out_weight, ffn_gain, ffn_gate_weight, ffn_up_weight, down_weight):

    def sequence_block(inputs):
        seq_count = inputs.shape[1]
        residual = inputs.reshape(-1, D).astype(jnp.float32)
        normed = rms_scale(residual, mix_gain).astype(jnp.bfloat16)
        value_rows = jnp.dot(normed, value_weight, preferred_element_type=jnp.float32)
        gate_rows = jnp.dot(normed, gate_weight, preferred_element_type=jnp.float32)
        glu_rows = (value_rows * jax.nn.sigmoid(gate_rows)).astype(jnp.bfloat16).reshape(LEN, seq_count, CH)
        conved = lax.conv_general_dilated(glu_rows.astype(jnp.float32), conv_taps[:, None, :], (1,), [(KW // 2, KW // 2)], dimension_numbers=('WNC', 'WIO', 'WNC'), feature_group_count=CH, precision=lax.Precision.HIGHEST)
        grouped = conved.reshape(LEN, seq_count, HEADS, HEAD_DIM)
        head_mean = lax.optimization_barrier(jnp.mean(grouped, axis=-1, keepdims=True))
        head_var = lax.optimization_barrier(jnp.mean(jnp.square(grouped - head_mean), axis=-1, keepdims=True))
        scaled = (grouped - head_mean) * lax.rsqrt(head_var + group_eps) * head_gain.reshape(HEADS, HEAD_DIM)
        activated = jax.nn.silu(scaled).astype(jnp.bfloat16).reshape(-1, CH)
        mixed_rows = split_sum(activated, out_weight, CH // N_TP)
        middle = (residual + mixed_rows).astype(jnp.bfloat16)
        middle_f = middle.astype(jnp.float32)
        normed_ffn = rms_scale(middle_f, ffn_gain).astype(jnp.bfloat16)
        gate_part = jnp.dot(normed_ffn, ffn_gate_weight, preferred_element_type=jnp.float32)
        up_part = jnp.dot(normed_ffn, ffn_up_weight, preferred_element_type=jnp.float32)
        hidden = (jax.nn.silu(gate_part) * up_part).astype(jnp.bfloat16)
        fed_rows = split_sum(hidden, down_weight, FF // N_TP)
        return (middle_f + fed_rows).astype(jnp.bfloat16).reshape(inputs.shape)
    blocks = tokens.reshape(LEN, BATCH // SEQ_DEV, SEQ_DEV, D).transpose(1, 0, 2, 3)
    results = lax.map(sequence_block, blocks)
    return results.transpose(1, 0, 2, 3).reshape(LEN, BATCH, D)
```

```python
import jax
import jax.numpy as jnp
from jax import lax
from jax.sharding import PartitionSpec as P

HEAD_DIM = 128

norm_eps = 1e-06
group_eps = 1e-05
f32 = jnp.float32
bf16 = jnp.bfloat16


def rms_scale(matrix, scales):
    return matrix * lax.rsqrt(jnp.mean(matrix * matrix, axis=-1, keepdims=True) + norm_eps) * scales


def body(
    tokens,
    mix_gain,
    value_weight,
    gate_weight,
    conv_taps,
    head_gain,
    out_weight,
    ffn_gain,
    ffn_gate_weight,
    ffn_up_weight,
    down_weight,
):
    n_rep, n_fs, n_tp = lax.axis_size("rep"), lax.axis_size("fs"), lax.axis_size("tp")
    rep, fs, tp = lax.axis_index("rep"), lax.axis_index("fs"), lax.axis_index("tp")
    ring = n_fs // 2
    pair, place = fs % 2, fs // 2
    local_len, seq_count, width = tokens.shape
    assert n_rep == 2 and n_tp == 2 and n_fs % 2 == 0 and seq_count == 1
    quarters = 2 * n_rep
    mine_q = rep * 2 + pair
    other_q = rep * 2 + 1 - pair

    flip_pair = [(i, i ^ 1) for i in range(n_fs)]
    flip_two = [(0, 1), (1, 0)]
    flip_both = [
        (r * n_fs + i, (1 - r) * n_fs + (i ^ 1)) for r in range(n_rep) for i in range(n_fs)
    ]
    step_ring = [(i, (i + 2) % n_fs) for i in range(n_fs)]

    def to_pair(a):
        return lax.ppermute(a, "fs", flip_pair)

    def to_rep(a):
        return lax.ppermute(a, "rep", flip_two)

    def to_both(a):
        return lax.ppermute(a, ("rep", "fs"), flip_both)

    def to_tp(a):
        return lax.ppermute(a, "tp", flip_two)

    def to_ring(a):
        return lax.ppermute(a, "fs", step_ring)

    def paired(weight, axis):
        size = weight.shape[axis] // quarters
        own = lax.dynamic_slice_in_dim(weight, mine_q * size, size, axis)
        got = to_pair(lax.dynamic_slice_in_dim(weight, other_q * size, size, axis))
        low = jnp.where(pair == 0, own, got)
        high = jnp.where(pair == 0, got, own)
        return jnp.concatenate([low, high], axis=1 - axis)

    history = []

    def hop(block):
        if len(history) >= 2:
            block, _ = lax.optimization_barrier((block, history[-2]))
        got = to_ring(block)
        history.append(got)
        return got

    def place_block(whole, block, step, axis):
        size = block.shape[axis]
        at = ((place + ring - step) % ring) * size
        return lax.dynamic_update_slice_in_dim(whole, block, at, axis)

    def gather_ring(weights, axes):
        blocks = [paired(w, a) for w, a in zip(weights, axes)]
        wholes = []
        for block, a in zip(blocks, axes):
            shape = list(block.shape)
            shape[1 - a] *= ring
            wholes.append(place_block(jnp.zeros(shape, block.dtype), block, 0, 1 - a))
        for step in range(1, ring):
            blocks = [hop(b) for b in blocks]
            wholes = [place_block(w, b, step, 1 - a) for w, b, a in zip(wholes, blocks, axes)]
        return wholes

    def gather_rows(own):
        near = [own, to_pair(own), to_rep(own), to_both(own)]
        far = [to_tp(a) for a in near]
        return jnp.concatenate(near + far, axis=0)

    def scatter_rows(near, far, weight):
        def product(a):
            return jnp.dot(a, weight, preferred_element_type=f32)

        sums = []
        for k in (3, 2, 1, 0):
            got = to_tp(product(far[k]).astype(bf16))
            part = product(near[k]) + got.astype(f32)
            if k == 0:
                sums.append(part)
            else:
                move = (None, to_pair, to_rep, to_both)[k]
                sums.append(move(part.astype(bf16)).astype(f32))
        return sums[0] + sums[1] + sums[2] + sums[3]

    rows = tokens.reshape(local_len, width)
    normed = gather_rows(rms_scale(rows.astype(f32), mix_gain).astype(bf16))
    value_q, gate_q = gather_ring((value_weight, gate_weight), (1, 1))
    (out_q,) = gather_ring((out_weight,), (0,))
    ffn_gate_q, ffn_up_q = gather_ring((ffn_gate_weight, ffn_up_weight), (1, 1))
    (down_q,) = gather_ring((down_weight,), (0,))

    value_rows = jnp.dot(normed, value_q, preferred_element_type=f32)
    gate_rows = jnp.dot(normed, gate_q, preferred_element_type=f32)
    glu = (value_rows * jax.nn.sigmoid(gate_rows)).astype(bf16)
    channels = glu.shape[1]
    glu = glu.reshape(2, 4, local_len, channels)
    first = jnp.where(tp == 0, glu[0], glu[1])
    second = jnp.where(tp == 0, glu[1], glu[0])
    sequence = jnp.concatenate([first, second], axis=1)
    taps = lax.dynamic_slice_in_dim(conv_taps, mine_q * channels, channels, 1)
    gains = lax.dynamic_slice_in_dim(head_gain, mine_q * channels, channels, 0)
    kernel = taps.shape[0]
    conved = lax.conv_general_dilated(
        sequence.astype(f32),
        taps[:, None, :],
        (1,),
        [(kernel // 2, kernel // 2)],
        dimension_numbers=("NWC", "WIO", "NWC"),
        feature_group_count=channels,
        precision=lax.Precision.HIGHEST,
    )
    grouped = conved.reshape(4, 2 * local_len, channels // HEAD_DIM, HEAD_DIM)
    head_mean = jnp.mean(grouped, axis=-1, keepdims=True)
    head_var = jnp.mean(jnp.square(grouped - head_mean), axis=-1, keepdims=True)
    scaled = (grouped - head_mean) * lax.rsqrt(head_var + group_eps) * gains.reshape(-1, HEAD_DIM)
    activated = jax.nn.silu(scaled).astype(bf16).reshape(4, 2 * local_len, channels)
    near = lax.dynamic_slice_in_dim(activated, tp * local_len, local_len, 1)
    far = lax.dynamic_slice_in_dim(activated, (1 - tp) * local_len, local_len, 1)
    mixed = scatter_rows(near, far, out_q)
    middle = (rows.astype(f32) + mixed).astype(bf16)
    middle_f = middle.astype(f32)
    normed_ffn = gather_rows(rms_scale(middle_f, ffn_gain).astype(bf16))
    gate_part = jnp.dot(normed_ffn, ffn_gate_q, preferred_element_type=f32)
    up_part = jnp.dot(normed_ffn, ffn_up_q, preferred_element_type=f32)
    hidden = (jax.nn.silu(gate_part) * up_part).astype(bf16)
    hidden = hidden.reshape(2, 4, local_len, -1)
    fed = scatter_rows(hidden[0], hidden[1], down_q)
    layer_rows = (middle_f + fed).astype(bf16)
    return layer_rows.reshape(local_len, seq_count, width)


def solution(mesh):
    placed = (
        P("tp", ("rep", "fs"), None),
        P(),
        P("fs", "tp"),
        P("fs", "tp"),
        P(None, "tp"),
        P("tp"),
        P("tp", "fs"),
        P(),
        P("fs", "tp"),
        P("fs", "tp"),
        P("tp", "fs"),
    )
    return jax.shard_map(
        body, mesh=mesh, in_specs=placed, out_specs=P("tp", ("rep", "fs"), None), check_vma=False
    )
```

```python
import functools

import jax
import jax.numpy as jnp
from jax import lax
from jax.experimental import pallas as pl
from jax.experimental.pallas import tpu as pltpu
from jax.sharding import PartitionSpec as P

HEAD_DIM = 128
MESH = pl.DeviceIdType.MESH

norm_eps = 1e-06
group_eps = 1e-05
f32 = jnp.float32
bf16 = jnp.bfloat16


def rms_scale(matrix, scales):
    return matrix * lax.rsqrt(jnp.mean(matrix * matrix, axis=-1, keepdims=True) + norm_eps) * scales


class Moves:
    def __init__(self, n_rep, n_fs, sources, wholes, axes, sems):
        self.rep, self.fs, self.tp = lax.axis_index("rep"), lax.axis_index("fs"), lax.axis_index("tp")
        rep, fs, tp = self.rep, self.fs, self.tp
        self.ring = n_fs // 2
        self.pair, self.place = fs % 2, fs // 2
        flip = fs + 1 - 2 * self.pair
        self.to_tp = (rep, fs, 1 - tp)
        self.peers = (None, (rep, flip, tp), (1 - rep, fs, tp), (1 - rep, flip, tp))
        self.after = (rep, (fs + 2) % n_fs, tp)
        self.before = (rep, (fs + n_fs - 2) % n_fs, tp)
        self.quarter = rep * 2 + self.pair
        self.other = rep * 2 + 1 - self.pair
        self.sources, self.wholes, self.axes = sources, wholes, axes
        self.ring_send, self.ring_recv, self.pair_send, self.pair_recv = sems

    def barrier(self):
        sem = pltpu.get_barrier_semaphore()
        others = self.peers[1:] + (self.to_tp, self.after, self.before)
        for device in others:
            pl.semaphore_signal(sem, inc=1, device_id=device, device_id_type=MESH)
        pl.semaphore_wait(sem, len(others))

    def part(self, w, quarter):
        size = self.sources[w].shape[self.axes[w]] // 4
        at = pl.ds(pl.multiple_of(quarter * size, size), size)
        return (slice(None), at) if self.axes[w] == 1 else (at, slice(None))

    def slot(self, w, owner):
        if self.axes[w] == 0:
            return (owner,)
        size = self.sources[w].shape[0]
        return (pl.ds(pl.multiple_of(owner * size, size), size), slice(None))

    def pair_copy(self, w):
        return pltpu.make_async_remote_copy(
            src_ref=self.sources[w].at[self.part(w, self.other)],
            dst_ref=self.wholes[w].at[self.slot(w, self.fs)],
            send_sem=self.pair_send.at[w],
            recv_sem=self.pair_recv.at[w],
            device_id=self.peers[1],
            device_id_type=MESH,
        )

    def ring_copy(self, w, p, s):
        parity = self.pair if p == 0 else 1 - self.pair
        owner = ((self.place + self.ring + 1 - s) % self.ring) * 2 + parity
        there = self.wholes[w].at[self.slot(w, owner)]
        here = self.sources[w].at[self.part(w, self.quarter)] if s == 1 and p == 0 else there
        return pltpu.make_async_remote_copy(
            src_ref=here,
            dst_ref=there,
            send_sem=self.ring_send.at[w, p, s - 1],
            recv_sem=self.ring_recv.at[w, p, s - 1],
            device_id=self.after,
            device_id_type=MESH,
        )

    def push(self, w, p, s):
        if s > 1:
            self.ring_copy(w, p, s - 1).wait_recv()
        elif p == 1:
            self.pair_copy(w).wait_recv()
        self.ring_copy(w, p, s).start()

    def arrived(self, w):
        for p in (0, 1):
            self.ring_copy(w, p, self.ring - 1).wait_recv()

    def sent(self):
        for w in range(len(self.sources)):
            self.pair_copy(w).wait_send()
            for p in (0, 1):
                for s in range(1, self.ring):
                    self.ring_copy(w, p, s).wait_send()

    def row_copy(self, src, dst, k, sems):
        return pltpu.make_async_remote_copy(
            src_ref=src,
            dst_ref=dst,
            send_sem=sems[0].at[k],
            recv_sem=sems[1].at[k],
            device_id=self.peers[k] if 0 < k < 4 else self.to_tp,
            device_id_type=MESH,
        )


def ring_scratch(count, n_fs):
    ring = n_fs // 2
    return [pltpu.SemaphoreType.DMA((count, 2, ring - 1))] * 2 + [pltpu.SemaphoreType.DMA((count,))] * 2


def whole_shapes(weights, axes, n_fs):
    shapes = []
    for weight, axis in zip(weights, axes):
        shape = list(weight.shape)
        shape[axis] //= 4
        shapes.append((shape[0] * n_fs, shape[1]) if axis == 1 else (n_fs, *shape))
    return shapes


def first_kernel(
    n_rep, n_fs, own, value, gate, out, rows, value_q, gate_q, out_q,
    ring_send, ring_recv, pair_send, pair_recv, row_send, row_recv, local_sem,
):
    sems = (ring_send, ring_recv, pair_send, pair_recv)
    m = Moves(n_rep, n_fs, (value, gate, out), (value_q, gate_q, out_q), (1, 1, 0), sems)
    row_sems = (row_send, row_recv)
    local = [pltpu.make_async_copy(own, rows.at[0], local_sem.at[3])]
    for w in range(3):
        local.append(
            pltpu.make_async_copy(
                m.sources[w].at[m.part(w, m.quarter)],
                m.wholes[w].at[m.slot(w, m.fs)],
                local_sem.at[w],
            )
        )
    for copy in local:
        copy.start()
    m.barrier()
    for w in range(3):
        m.pair_copy(w).start()
        m.push(w, 0, 1)
    near = {k: m.row_copy(own, rows.at[k], k, row_sems) for k in (1, 2, 3)}
    far = {
        k: m.row_copy(own if k == 0 else rows.at[k], rows.at[4 + k], 4 + k, row_sems)
        for k in (0, 1, 2, 3)
    }
    near[3].start()
    near[1].start()
    near[2].start()
    far[0].start()
    for w in range(3):
        m.push(w, 1, 1)
    for s in range(2, m.ring):
        for p in (0, 1):
            for w in range(3):
                m.push(w, p, s)
    for k in (1, 2, 3):
        near[k].wait_recv()
        far[k].start()
    for w in range(3):
        m.arrived(w)
    for k in range(4):
        far[k].wait_recv()
    for copy in local:
        copy.wait()
    for copy in list(near.values()) + list(far.values()):
        copy.wait_send()
    m.sent()


def second_kernel(
    n_rep, n_fs, tokens, act_near, act_far, out_q, ffn_gain, gate, up, down, result,
    gate_q, up_q, down_q, rows, hidden, middle, total, tp_out, tp_in, x_out, x_in,
    ring_send, ring_recv, pair_send, pair_recv, row_send, row_recv, sum_send, sum_recv,
):
    sems = (ring_send, ring_recv, pair_send, pair_recv)
    m = Moves(n_rep, n_fs, (gate, up, down), (gate_q, up_q, down_q), (1, 1, 0), sems)
    row_sems = (row_send, row_recv)
    length, width = tokens.shape
    tile = 512
    high = 32
    m.barrier()
    for w in range(3):
        m.pair_copy(w).start()
    for w in range(2):
        m.push(w, 0, 1)

    def columns(weight, c):
        slots = tile // weight.shape[2]
        return jnp.concatenate([weight[c * slots + i] for i in range(slots)], axis=1)

    def far_sums(phase, far, weight):
        for k in (3, 1, 2, 0):

            def column(c, _):
                at = pl.ds(pl.multiple_of(c * tile, tile), tile)
                tp_out[phase, k, :, at] = jnp.dot(
                    far(k), columns(weight, c), preferred_element_type=f32
                ).astype(bf16)
                return _

            lax.fori_loop(0, width // tile, column, 0)
            tp_copy(phase, k).start()

    def tp_copy(phase, k):
        return m.row_copy(
            tp_out.at[phase, k], tp_in.at[phase, k], 4 + k, (sum_send.at[phase], sum_recv.at[phase])
        )

    def x_copy(phase, k):
        return m.row_copy(
            x_out.at[phase, k - 1], x_in.at[phase, k - 1], k, (sum_send.at[phase], sum_recv.at[phase])
        )

    def near_sums(phase, near, weight):
        for k in (3, 1, 2, 0):
            tp_copy(phase, k).wait_recv()

            def column(c, _):
                at = pl.ds(pl.multiple_of(c * tile, tile), tile)
                part = jnp.dot(near(k), columns(weight, c), preferred_element_type=f32)
                part = part + tp_in[phase, k, :, at].astype(f32)
                if k == 0:
                    total[:, at] = part
                else:
                    x_out[phase, k - 1, :, at] = part.astype(bf16)
                return _

            lax.fori_loop(0, width // tile, column, 0)
            if k:
                x_copy(phase, k).start()

    def all_sums(phase, at):
        part = total[at, :]
        for k in (1, 2, 3):
            part = part + x_in[phase, k - 1, at, :].astype(f32)
        return part

    far_sums(0, lambda k: act_far[k], out_q)
    for w in range(2):
        m.push(w, 1, 1)
    near_sums(0, lambda k: act_near[k], out_q)
    for w in range(3):
        m.wholes[w][m.slot(w, m.fs)] = m.sources[w][m.part(w, m.quarter)]
    for w in range(2):
        m.push(w, 0, 2)
    for w in range(2):
        m.push(w, 1, 2)
    for k in (1, 2, 3):
        x_copy(0, k).wait_recv()

    def norm_rows(i, _):
        at = pl.ds(pl.multiple_of(i * high, high), high)
        mid = (tokens[at, :].astype(f32) + all_sums(0, at)).astype(bf16)
        middle[at, :] = mid
        rows[0, at, :] = rms_scale(mid.astype(f32), ffn_gain[...]).astype(bf16)
        return _

    lax.fori_loop(0, length // high, norm_rows, 0)
    near = {k: m.row_copy(rows.at[0], rows.at[k], k, row_sems) for k in (1, 2, 3)}
    far = {k: m.row_copy(rows.at[k], rows.at[4 + k], 4 + k, row_sems) for k in (0, 1, 2, 3)}
    near[3].start()
    near[1].start()
    near[2].start()
    far[0].start()
    for s in range(3, m.ring):
        for p in (0, 1):
            for w in range(2):
                m.push(w, p, s)
    for p in (0, 1):
        m.push(2, p, 1)
    for k in (1, 2, 3):
        near[k].wait_recv()
        far[k].start()
    for w in range(2):
        m.arrived(w)
    m.push(2, 0, 2)
    for k in range(4):
        far[k].wait_recv()

    def feed(i, _):
        at = pl.ds(2 * i, 2)
        block = rows[at].reshape(2 * length, width)
        gate_part = jnp.dot(block, gate_q[...], preferred_element_type=f32)
        up_part = jnp.dot(block, up_q[...], preferred_element_type=f32)
        hidden[at] = (jax.nn.silu(gate_part) * up_part).astype(bf16).reshape(2, length, -1)
        return _

    lax.fori_loop(0, 4, feed, 0)
    m.push(2, 1, 2)
    for s in range(3, m.ring):
        for p in (0, 1):
            m.push(2, p, s)
    m.arrived(2)
    far_sums(1, lambda k: hidden[4 + k], down_q)
    near_sums(1, lambda k: hidden[k], down_q)
    for k in (1, 2, 3):
        x_copy(1, k).wait_recv()

    def finish(i, _):
        at = pl.ds(pl.multiple_of(i * high, high), high)
        result[at, :] = (middle[at, :].astype(f32) + all_sums(1, at)).astype(bf16)
        return _

    lax.fori_loop(0, length // high, finish, 0)
    for copy in list(near.values()) + list(far.values()):
        copy.wait_send()
    for phase in (0, 1):
        for k in range(4):
            tp_copy(phase, k).wait_send()
        for k in (1, 2, 3):
            x_copy(phase, k).wait_send()
    m.sent()


def body(
    tokens,
    mix_gain,
    value_weight,
    gate_weight,
    conv_taps,
    head_gain,
    out_weight,
    ffn_gain,
    ffn_gate_weight,
    ffn_up_weight,
    down_weight,
):
    n_rep, n_fs, n_tp = lax.axis_size("rep"), lax.axis_size("fs"), lax.axis_size("tp")
    rep, fs, tp = lax.axis_index("rep"), lax.axis_index("fs"), lax.axis_index("tp")
    pair = fs % 2
    local_len, seq_count, width = tokens.shape
    assert n_rep == 2 and n_tp == 2 and n_fs % 2 == 0 and seq_count == 1
    mine_q = rep * 2 + pair
    vmem, anywhere = pl.BlockSpec(memory_space=pltpu.VMEM), pl.BlockSpec(memory_space=pl.ANY)
    sem = pltpu.SemaphoreType.DMA

    rows = tokens.reshape(local_len, width)
    own = rms_scale(rows.astype(f32), mix_gain).astype(bf16)
    module_weights = (value_weight, gate_weight, out_weight)
    shapes = whole_shapes(module_weights, (1, 1, 0), n_fs)
    normed, value_q, gate_q, out_q = pl.pallas_call(
        functools.partial(first_kernel, n_rep, n_fs),
        out_shape=[jax.ShapeDtypeStruct(s, bf16) for s in [(8, local_len, width)] + shapes],
        in_specs=[vmem] * 4,
        out_specs=[anywhere] * 4,
        scratch_shapes=ring_scratch(3, n_fs) + [sem((8,)), sem((8,)), sem((4,))],
        compiler_params=pltpu.CompilerParams(collective_id=0, has_side_effects=True),
    )(own, *module_weights)
    normed = normed.reshape(8 * local_len, width)

    value_rows = jnp.dot(normed, value_q, preferred_element_type=f32)
    gate_rows = jnp.dot(normed, gate_q, preferred_element_type=f32)
    glu = (value_rows * jax.nn.sigmoid(gate_rows)).astype(bf16)
    channels = glu.shape[1]
    glu = glu.reshape(2, 4, local_len, channels)
    first = jnp.where(tp == 0, glu[0], glu[1])
    second = jnp.where(tp == 0, glu[1], glu[0])
    sequence = jnp.concatenate([first, second], axis=1)
    taps = lax.dynamic_slice_in_dim(conv_taps, mine_q * channels, channels, 1)
    gains = lax.dynamic_slice_in_dim(head_gain, mine_q * channels, channels, 0)
    kernel = taps.shape[0]
    conved = lax.conv_general_dilated(
        sequence.astype(f32),
        taps[:, None, :],
        (1,),
        [(kernel // 2, kernel // 2)],
        dimension_numbers=("NWC", "WIO", "NWC"),
        feature_group_count=channels,
        precision=lax.Precision.HIGHEST,
    )
    grouped = conved.reshape(4, 2 * local_len, channels // HEAD_DIM, HEAD_DIM)
    head_mean = jnp.mean(grouped, axis=-1, keepdims=True)
    head_var = jnp.mean(jnp.square(grouped - head_mean), axis=-1, keepdims=True)
    scaled = (grouped - head_mean) * lax.rsqrt(head_var + group_eps) * gains.reshape(-1, HEAD_DIM)
    activated = jax.nn.silu(scaled).astype(bf16).reshape(4, 2 * local_len, channels)
    near = lax.dynamic_slice_in_dim(activated, tp * local_len, local_len, 1)
    far = lax.dynamic_slice_in_dim(activated, (1 - tp) * local_len, local_len, 1)
    ffn_weights = (ffn_gate_weight, ffn_up_weight, down_weight)
    shapes = whole_shapes(ffn_weights, (1, 1, 0), n_fs)
    units = shapes[0][1]
    layer_rows = pl.pallas_call(
        functools.partial(second_kernel, n_rep, n_fs),
        out_shape=jax.ShapeDtypeStruct((local_len, width), bf16),
        in_specs=[vmem] * 8,
        out_specs=vmem,
        scratch_shapes=[pltpu.VMEM(s, bf16) for s in shapes]
        + [
            pltpu.VMEM((8, local_len, width), bf16),
            pltpu.VMEM((8, local_len, units), bf16),
            pltpu.VMEM((local_len, width), bf16),
            pltpu.VMEM((local_len, width), f32),
            pltpu.VMEM((2, 4, local_len, width), bf16),
            pltpu.VMEM((2, 4, local_len, width), bf16),
            pltpu.VMEM((2, 3, local_len, width), bf16),
            pltpu.VMEM((2, 3, local_len, width), bf16),
        ]
        + ring_scratch(3, n_fs)
        + [sem((8,)), sem((8,)), sem((2, 8)), sem((2, 8))],
        compiler_params=pltpu.CompilerParams(
            collective_id=1, has_side_effects=True, vmem_limit_bytes=56 * 1024 * 1024
        ),
    )(rows, near, far, out_q, ffn_gain.reshape(1, width), *ffn_weights)
    return layer_rows.reshape(local_len, seq_count, width)


def solution(mesh):
    placed = (
        P("tp", ("rep", "fs"), None),
        P(),
        P("fs", "tp"),
        P("fs", "tp"),
        P(None, "tp"),
        P("tp"),
        P("tp", "fs"),
        P(),
        P("fs", "tp"),
        P("fs", "tp"),
        P("tp", "fs"),
    )
    return jax.shard_map(
        body, mesh=mesh, in_specs=placed, out_specs=P("tp", ("rep", "fs"), None), check_vma=False
    )
```

```python
import functools

import jax
import jax.numpy as jnp
from jax import lax
from jax.experimental import pallas as pl
from jax.experimental.pallas import tpu as pltpu
from jax.sharding import PartitionSpec as P

HEAD_DIM = 128
MESH = pl.DeviceIdType.MESH

norm_eps = 1e-06
group_eps = 1e-05
f32 = jnp.float32
bf16 = jnp.bfloat16


def rms_scale(matrix, scales):
    return matrix * lax.rsqrt(jnp.mean(matrix * matrix, axis=-1, keepdims=True) + norm_eps) * scales


class Moves:
    def __init__(self, n_rep, n_fs, sources, wholes, axes, sems):
        self.rep, self.fs, self.tp = lax.axis_index("rep"), lax.axis_index("fs"), lax.axis_index("tp")
        rep, fs, tp = self.rep, self.fs, self.tp
        self.ring = n_fs // 2
        self.pair, self.place = fs % 2, fs // 2
        flip = fs + 1 - 2 * self.pair
        self.to_tp = (rep, fs, 1 - tp)
        self.peers = (None, (rep, flip, tp), (1 - rep, fs, tp), (1 - rep, flip, tp))
        self.after = (rep, (fs + 2) % n_fs, tp)
        self.before = (rep, (fs + n_fs - 2) % n_fs, tp)
        self.quarter = rep * 2 + self.pair
        self.other = rep * 2 + 1 - self.pair
        self.sources, self.wholes, self.axes = sources, wholes, axes
        self.ring_send, self.ring_recv, self.pair_send, self.pair_recv = sems

    def barrier(self):
        sem = pltpu.get_barrier_semaphore()
        others = self.peers[1:] + (self.to_tp, self.after, self.before)
        for device in others:
            pl.semaphore_signal(sem, inc=1, device_id=device, device_id_type=MESH)
        pl.semaphore_wait(sem, len(others))

    def part(self, w, quarter):
        size = self.sources[w].shape[self.axes[w]] // 4
        at = pl.ds(pl.multiple_of(quarter * size, size), size)
        return (slice(None), at) if self.axes[w] == 1 else (at, slice(None))

    def slot(self, w, owner):
        if self.axes[w] == 0:
            return (owner,)
        size = self.sources[w].shape[0]
        return (pl.ds(pl.multiple_of(owner * size, size), size), slice(None))

    def pair_copy(self, w):
        return pltpu.make_async_remote_copy(
            src_ref=self.sources[w].at[self.part(w, self.other)],
            dst_ref=self.wholes[w].at[self.slot(w, self.fs)],
            send_sem=self.pair_send.at[w],
            recv_sem=self.pair_recv.at[w],
            device_id=self.peers[1],
            device_id_type=MESH,
        )

    def ring_copy(self, w, p, s):
        parity = self.pair if p == 0 else 1 - self.pair
        owner = ((self.place + self.ring + 1 - s) % self.ring) * 2 + parity
        there = self.wholes[w].at[self.slot(w, owner)]
        here = self.sources[w].at[self.part(w, self.quarter)] if s == 1 and p == 0 else there
        return pltpu.make_async_remote_copy(
            src_ref=here,
            dst_ref=there,
            send_sem=self.ring_send.at[w, p, s - 1],
            recv_sem=self.ring_recv.at[w, p, s - 1],
            device_id=self.after,
            device_id_type=MESH,
        )

    def push(self, w, p, s):
        if s > 1:
            self.ring_copy(w, p, s - 1).wait_recv()
        elif p == 1:
            self.pair_copy(w).wait_recv()
        self.ring_copy(w, p, s).start()

    def arrived(self, w):
        for p in (0, 1):
            self.ring_copy(w, p, self.ring - 1).wait_recv()

    def sent(self):
        for w in range(len(self.sources)):
            self.pair_copy(w).wait_send()
            for p in (0, 1):
                for s in range(1, self.ring):
                    self.ring_copy(w, p, s).wait_send()

    def copy(self, src, dst, device, sems, i):
        return pltpu.make_async_remote_copy(
            src_ref=src,
            dst_ref=dst,
            send_sem=sems[0].at[i],
            recv_sem=sems[1].at[i],
            device_id=device,
            device_id_type=MESH,
        )


class RowGather:
    def __init__(self, m, own, rows, sems):
        half = own.shape[0] // 2
        low, high = pl.ds(0, half), pl.ds(half, half)
        _, pair, rep, _ = m.peers
        moves = (
            (own.at[low], rows.at[2, low], rep),
            (own.at[high], rows.at[1, high], pair),
            (own.at[high], rows.at[2, high], rep),
            (own.at[low], rows.at[1, low], pair),
            (rows.at[2, low], rows.at[3, low], pair),
            (rows.at[1, high], rows.at[3, high], rep),
            (own, rows.at[4], m.to_tp),
            (rows.at[2], rows.at[6], m.to_tp),
            (rows.at[1], rows.at[5], m.to_tp),
            (rows.at[3, low], rows.at[7, low], m.to_tp),
            (rows.at[3, high], rows.at[7, high], m.to_tp),
        )
        self.copies = [m.copy(*move, sems, i) for i, move in enumerate(moves)]

    def start(self):
        for i in (0, 1, 2, 3, 6):
            self.copies[i].start()

    def forward(self):
        for i in (0, 1):
            self.copies[i].wait_recv()
            self.copies[i + 4].start()

    def finish(self):
        for i in (2, 3, 4, 5):
            self.copies[i].wait_recv()
            self.copies[i + 5].start()

    def arrived(self):
        for i in range(6, 11):
            self.copies[i].wait_recv()

    def sent(self):
        for copy in self.copies:
            copy.wait_send()


def ring_scratch(count, n_fs):
    ring = n_fs // 2
    return [pltpu.SemaphoreType.DMA((count, 2, ring - 1))] * 2 + [pltpu.SemaphoreType.DMA((count,))] * 2


def whole_shapes(weights, axes, n_fs):
    shapes = []
    for weight, axis in zip(weights, axes):
        shape = list(weight.shape)
        shape[axis] //= 4
        shapes.append((shape[0] * n_fs, shape[1]) if axis == 1 else (n_fs, *shape))
    return shapes


def first_kernel(
    n_rep, n_fs, own, value, gate, out, rows, value_q, gate_q, out_q,
    ring_send, ring_recv, pair_send, pair_recv, row_send, row_recv, local_sem,
):
    sems = (ring_send, ring_recv, pair_send, pair_recv)
    m = Moves(n_rep, n_fs, (value, gate, out), (value_q, gate_q, out_q), (1, 1, 0), sems)
    row_sems = (row_send, row_recv)
    local = [pltpu.make_async_copy(own, rows.at[0], local_sem.at[3])]
    for w in range(3):
        local.append(
            pltpu.make_async_copy(
                m.sources[w].at[m.part(w, m.quarter)],
                m.wholes[w].at[m.slot(w, m.fs)],
                local_sem.at[w],
            )
        )
    for copy in local:
        copy.start()
    m.barrier()
    for w in range(3):
        m.pair_copy(w).start()
        m.push(w, 0, 1)
    gather = RowGather(m, own, rows, row_sems)
    gather.start()
    for w in range(3):
        m.push(w, 1, 1)
    gather.forward()
    for s in range(2, m.ring):
        for p in (0, 1):
            for w in range(3):
                m.push(w, p, s)
    gather.finish()
    for w in range(3):
        m.arrived(w)
    gather.arrived()
    for copy in local:
        copy.wait()
    gather.sent()
    m.sent()


def second_kernel(
    n_rep, n_fs, tokens, act_near, act_far, out_q, ffn_gain, gate, up, down, result,
    gate_q, up_q, down_q, rows, hidden, middle, total, tp_out, tp_in, x_out, x_in,
    ring_send, ring_recv, pair_send, pair_recv, row_send, row_recv, sum_send, sum_recv,
):
    sems = (ring_send, ring_recv, pair_send, pair_recv)
    m = Moves(n_rep, n_fs, (gate, up, down), (gate_q, up_q, down_q), (1, 1, 0), sems)
    row_sems = (row_send, row_recv)
    length, width = tokens.shape
    tile = 512
    high = 32
    m.barrier()
    for w in range(3):
        m.pair_copy(w).start()
    for w in range(2):
        m.push(w, 0, 1)

    def columns(weight, c):
        slots = tile // weight.shape[2]
        return jnp.concatenate([weight[c * slots + i] for i in range(slots)], axis=1)

    def tile_loop(step):
        def run(c, _):
            step(columns(out_q, c), pl.ds(pl.multiple_of(c * tile, tile), tile))
            return _

        lax.fori_loop(0, width // tile, run, 0)

    def phase_columns(phase):
        if phase == 0:
            return slice(None)
        size = 2 * width // n_fs
        owner = (m.place + m.ring + 1 - phase) % m.ring
        return pl.ds(pl.multiple_of(owner * size, size), size)

    def for_columns(phase, step):
        if phase == 0:
            tile_loop(step)
        else:
            owner = ((m.place + m.ring + 1 - phase) % m.ring) * 2
            weight = jnp.concatenate([down_q[owner], down_q[owner + 1]], axis=1)
            step(weight, phase_columns(phase))

    def tp_copy(phase, k):
        b, at = min(phase, 1), phase_columns(phase)
        phase_sems = (sum_send.at[phase], sum_recv.at[phase])
        return m.copy(tp_out.at[b, k, :, at], tp_in.at[b, k, :, at], m.to_tp, phase_sems, k)

    def x_copy(phase, k, low):
        b, columns_at = min(phase, 1), phase_columns(phase)
        at = pl.ds(0, length // 2) if low else pl.ds(length // 2, length // 2)
        to_rep = k == 2 or (k == 3 and low)
        return m.copy(
            x_out.at[b, k - 1, at, columns_at],
            x_in.at[b, k - 1, at, columns_at],
            m.peers[2 if to_rep else 1],
            (sum_send.at[phase], sum_recv.at[phase]),
            2 * k + 2 + low,
        )

    def far_sums(phase, far):
        b = min(phase, 1)
        for k in (3, 2, 1, 0):

            def step(weight, at):
                product = jnp.dot(far(k), weight, preferred_element_type=f32)
                tp_out[b, k, :, at] = product.astype(bf16)

            for_columns(phase, step)
            tp_copy(phase, k).start()

    def near_sums(phase, near):
        b = min(phase, 1)
        for k in (3, 2, 1, 0):
            tp_copy(phase, k).wait_recv()

            def step(weight, at):
                part = jnp.dot(near(k), weight, preferred_element_type=f32)
                part = part + tp_in[b, k, :, at].astype(f32)
                if k == 0:
                    total[b, :, at] = part
                else:
                    x_out[b, k - 1, :, at] = part.astype(bf16)

            for_columns(phase, step)
            if k == 3:
                x_copy(phase, 3, 1).start()
                x_copy(phase, 3, 0).start()
            elif k:
                x_copy(phase, k, k - 1).start()

    def forward_sums(phase):
        b, columns_at = min(phase, 1), phase_columns(phase)
        for k, low in ((1, 1), (2, 0)):
            x_copy(phase, 3, low).wait_recv()
            first = 0 if low else length // 2

            def add(i, _):
                at = pl.ds(pl.multiple_of(first + i * high, high), high)
                part = x_out[b, k - 1, at, columns_at].astype(f32)
                part = part + x_in[b, 2, at, columns_at].astype(f32)
                x_out[b, k - 1, at, columns_at] = part.astype(bf16)
                return _

            lax.fori_loop(0, length // (2 * high), add, 0)
            x_copy(phase, k, low).start()

    def sums_arrived(phase):
        for k in (1, 2):
            for low in (0, 1):
                x_copy(phase, k, low).wait_recv()

    def all_sums(b, at):
        part = total[b, at, :]
        for k in (1, 2):
            part = part + x_in[b, k - 1, at, :].astype(f32)
        return part

    far_sums(0, lambda k: act_far[k])
    for w in range(2):
        m.push(w, 1, 1)
    near_sums(0, lambda k: act_near[k])
    for w in range(3):
        m.wholes[w][m.slot(w, m.fs)] = m.sources[w][m.part(w, m.quarter)]
    for w in range(2):
        m.push(w, 0, 2)
    forward_sums(0)
    for w in range(2):
        m.push(w, 1, 2)
    sums_arrived(0)

    def norm_rows(i, _):
        at = pl.ds(pl.multiple_of(i * high, high), high)
        mid = (tokens[at, :].astype(f32) + all_sums(0, at)).astype(bf16)
        middle[at, :] = mid
        rows[0, at, :] = rms_scale(mid.astype(f32), ffn_gain[...]).astype(bf16)
        return _

    lax.fori_loop(0, length // high, norm_rows, 0)
    gather = RowGather(m, rows.at[0], rows, row_sems)
    gather.start()
    for s in range(3, m.ring):
        for p in (0, 1):
            for w in range(2):
                m.push(w, p, s)
            if s == 3 and p == 0:
                gather.forward()
    if m.ring < 4:
        gather.forward()
    for p in (0, 1):
        m.push(2, p, 1)
    gather.finish()
    for w in range(2):
        m.arrived(w)
    m.push(2, 0, 2)
    gather.arrived()

    def feed(i, _):
        at = pl.ds(2 * i, 2)
        block = rows[at].reshape(2 * length, width)
        gate_part = jnp.dot(block, gate_q[...], preferred_element_type=f32)
        up_part = jnp.dot(block, up_q[...], preferred_element_type=f32)
        hidden[at] = (jax.nn.silu(gate_part) * up_part).astype(bf16).reshape(2, length, -1)
        return _

    lax.fori_loop(0, 4, feed, 0)
    m.push(2, 1, 2)
    for t in range(m.ring):
        if t == m.ring - 1:
            m.arrived(2)
        elif t > 1:
            for p in (0, 1):
                m.push(2, p, t + 1)
        far_sums(1 + t, lambda k: hidden[4 + k])
        near_sums(1 + t, lambda k: hidden[k])
        if t:
            forward_sums(t)
    forward_sums(m.ring)
    for t in range(m.ring):
        sums_arrived(1 + t)

    def finish(i, _):
        at = pl.ds(pl.multiple_of(i * high, high), high)
        result[at, :] = (middle[at, :].astype(f32) + all_sums(1, at)).astype(bf16)
        return _

    lax.fori_loop(0, length // high, finish, 0)
    gather.sent()
    for phase in range(1 + m.ring):
        for k in range(4):
            tp_copy(phase, k).wait_send()
        for k in (1, 2, 3):
            for low in (0, 1):
                x_copy(phase, k, low).wait_send()
    m.sent()


def body(
    tokens,
    mix_gain,
    value_weight,
    gate_weight,
    conv_taps,
    head_gain,
    out_weight,
    ffn_gain,
    ffn_gate_weight,
    ffn_up_weight,
    down_weight,
):
    n_rep, n_fs, n_tp = lax.axis_size("rep"), lax.axis_size("fs"), lax.axis_size("tp")
    rep, fs, tp = lax.axis_index("rep"), lax.axis_index("fs"), lax.axis_index("tp")
    pair = fs % 2
    local_len, seq_count, width = tokens.shape
    assert n_rep == 2 and n_tp == 2 and n_fs % 2 == 0 and seq_count == 1
    mine_q = rep * 2 + pair
    vmem, anywhere = pl.BlockSpec(memory_space=pltpu.VMEM), pl.BlockSpec(memory_space=pl.ANY)
    sem = pltpu.SemaphoreType.DMA

    rows = tokens.reshape(local_len, width)
    own = rms_scale(rows.astype(f32), mix_gain).astype(bf16)
    module_weights = (value_weight, gate_weight, out_weight)
    shapes = whole_shapes(module_weights, (1, 1, 0), n_fs)
    normed, value_q, gate_q, out_q = pl.pallas_call(
        functools.partial(first_kernel, n_rep, n_fs),
        out_shape=[jax.ShapeDtypeStruct(s, bf16) for s in [(8, local_len, width)] + shapes],
        in_specs=[vmem] * 4,
        out_specs=[anywhere] * 4,
        scratch_shapes=ring_scratch(3, n_fs) + [sem((11,)), sem((11,)), sem((4,))],
        compiler_params=pltpu.CompilerParams(collective_id=0, has_side_effects=True),
    )(own, *module_weights)
    normed = normed.reshape(8 * local_len, width)

    value_rows = jnp.dot(normed, value_q, preferred_element_type=f32)
    gate_rows = jnp.dot(normed, gate_q, preferred_element_type=f32)
    glu = (value_rows * jax.nn.sigmoid(gate_rows)).astype(bf16)
    channels = glu.shape[1]
    glu = glu.reshape(2, 4, local_len, channels)
    first = jnp.where(tp == 0, glu[0], glu[1])
    second = jnp.where(tp == 0, glu[1], glu[0])
    sequence = jnp.concatenate([first, second], axis=1)
    taps = lax.dynamic_slice_in_dim(conv_taps, mine_q * channels, channels, 1)
    gains = lax.dynamic_slice_in_dim(head_gain, mine_q * channels, channels, 0)
    kernel = taps.shape[0]
    conved = lax.conv_general_dilated(
        sequence.astype(f32),
        taps[:, None, :],
        (1,),
        [(kernel // 2, kernel // 2)],
        dimension_numbers=("NWC", "WIO", "NWC"),
        feature_group_count=channels,
        precision=lax.Precision.HIGHEST,
    )
    grouped = conved.reshape(4, 2 * local_len, channels // HEAD_DIM, HEAD_DIM)
    head_mean = jnp.mean(grouped, axis=-1, keepdims=True)
    head_var = jnp.mean(jnp.square(grouped - head_mean), axis=-1, keepdims=True)
    scaled = (grouped - head_mean) * lax.rsqrt(head_var + group_eps) * gains.reshape(-1, HEAD_DIM)
    activated = jax.nn.silu(scaled).astype(bf16).reshape(4, 2 * local_len, channels)
    near = lax.dynamic_slice_in_dim(activated, tp * local_len, local_len, 1)
    far = lax.dynamic_slice_in_dim(activated, (1 - tp) * local_len, local_len, 1)
    ffn_weights = (ffn_gate_weight, ffn_up_weight, down_weight)
    shapes = whole_shapes(ffn_weights, (1, 1, 0), n_fs)
    units = shapes[0][1]
    layer_rows = pl.pallas_call(
        functools.partial(second_kernel, n_rep, n_fs),
        out_shape=jax.ShapeDtypeStruct((local_len, width), bf16),
        in_specs=[vmem] * 8,
        out_specs=vmem,
        scratch_shapes=[pltpu.VMEM(s, bf16) for s in shapes]
        + [
            pltpu.VMEM((8, local_len, width), bf16),
            pltpu.VMEM((8, local_len, units), bf16),
            pltpu.VMEM((local_len, width), bf16),
            pltpu.VMEM((2, local_len, width), f32),
            pltpu.VMEM((2, 4, local_len, width), bf16),
            pltpu.VMEM((2, 4, local_len, width), bf16),
            pltpu.VMEM((2, 3, local_len, width), bf16),
            pltpu.VMEM((2, 3, local_len, width), bf16),
        ]
        + ring_scratch(3, n_fs)
        + [sem((11,)), sem((11,)), sem((1 + n_fs // 2, 10)), sem((1 + n_fs // 2, 10))],
        compiler_params=pltpu.CompilerParams(
            collective_id=1, has_side_effects=True, vmem_limit_bytes=56 * 1024 * 1024
        ),
    )(rows, near, far, out_q, ffn_gain.reshape(1, width), *ffn_weights)
    return layer_rows.reshape(local_len, seq_count, width)


def solution(mesh):
    placed = (
        P("tp", ("rep", "fs"), None),
        P(),
        P("fs", "tp"),
        P("fs", "tp"),
        P(None, "tp"),
        P("tp"),
        P("tp", "fs"),
        P(),
        P("fs", "tp"),
        P("fs", "tp"),
        P("tp", "fs"),
    )
    return jax.shard_map(
        body, mesh=mesh, in_specs=placed, out_specs=P("tp", ("rep", "fs"), None), check_vma=False
    )
```
